32 devices in a mesh: ep: 8 (over z, y), tp: 4 (over x, core).
Axes of the slice: x: 2, y: 2, z: 4, core: 2. Of those that a mesh axis runs over, the one named last changes fastest.
Arguments:
- queries: bfloat16 [4096, 1024], P('ep', 'tp'), may hold values from -6 to 6
- keys: bfloat16 [4096, 512], P('ep', 'tp'), may hold values from -6 to 6
- values: bfloat16 [4096, 512], P('ep', 'tp'), may hold values from -6 to 6
- forget_cache: float32 [8, 4096], P('tp'), may hold values from -412 to 0, as said below
- query_gain: float32 [128], replicated, may hold values from 0.6 to 6
- key_gain: float32 [128], replicated, may hold values from 0.6 to 6
- mixer_out: bfloat16 [1024, 2048], replicated, may hold values from -0.75 to 0.75
- expert_input: bfloat16 [4096, 2048], P(('ep', 'tp')), may hold values from -6 to 6
- norm_gain: float32 [2048], replicated, may hold values from 0.1 to 1.9
- routes: int32 [4096, 2], P(('ep', 'tp')), may hold values from 0 to 31, all different within a row; in each aligned block of 128 rows (0 to 127, 128 to 255, ...) at most 16 rows name the same one
- route_weights: float32 [4096, 2], P(('ep', 'tp')), may hold values from 0.1 to 1
- w_gate: bfloat16 [32, 2048, 1024], P('ep', None, 'tp'), may hold values from -0.125 to 0.125
- w_up: bfloat16 [32, 2048, 1024], P('ep', None, 'tp'), may hold values from -0.125 to 0.125
- w_down: bfloat16 [32, 2048, 1024], P('ep', None, 'tp'), may hold values from -0.1875 to 0.1875
Outputs:
- mixed: bfloat16 [4096, 2048], P(('ep', 'tp'))
- routed: bfloat16 [4096, 2048], P(('ep', 'tp'))
The draws below stay inside these ranges and needn't reach their ends.
Inputs may be any that keep to these rules, and one draw needn't show every extreme that they name: `routes`: each row names 2 different experts; among the rows of one device no expert is named by more than 16 rows, a bound that some block reaches. `forget_cache`: never rises along the positions.
All inputs are finite; a program needn't handle non-finite values.
Results may differ from the reference program's by a relative error of at most 0.013.
The reference program's roundings to bfloat16 on the way count: a program that leaves them out, or rounds other values in their place, can miss the bound.
Values may be sent and summed in bfloat16 or wider, within the bound.
No kernel may reach another device: no remote copies, remote signals or barrier semaphores. Data moves between devices by JAX's collectives and lax.ppermute only.
A program may use at most 128 MiB of HBM per device.

```python
import math
import jax
import jax.numpy as jnp
import numpy as np
from jax import lax

D = 2048
QUERY_HEADS = 8
KV_HEADS = 4
HD = 128
EXPERTS = 32
TOPK = 2
FF = 1024
TB_DEV = 128
CAP = 16
ATTENTION_TOKENS = 4096
TOK_B = 4096
N_EP = 8
N_TP = 4


def draw_forget_cache(key, part):
    parallel_flows = jax.random.split(jax.random.fold_in(key, 11), 5)
    token_positions = jnp.arange(ATTENTION_TOKENS, dtype=jnp.int32)
    order = jax.random.permutation(parallel_flows[0], QUERY_HEADS)
    quick = order < QUERY_HEADS // 2
    rate = jnp.where(quick, 1.0 / 40.0, 0.8 / ATTENTION_TOKENS)
    rough = jax.random.uniform(parallel_flows[1], (QUERY_HEADS, ATTENTION_TOKENS), jnp.float32, 0.3, 1.7)
    blocks = 16
    factor = jnp.exp(jax.random.uniform(parallel_flows[2], (QUERY_HEADS, blocks), jnp.float32, -0.7, 0.7))
    which = token_positions * blocks // ATTENTION_TOKENS
    steps = -rate[:, None] * rough * factor[:, which]
    token_groups = jax.random.randint(parallel_flows[3], (QUERY_HEADS, 3), 0, ATTENTION_TOKENS)
    depth = jnp.log(jax.random.uniform(parallel_flows[4], (QUERY_HEADS, 3), jnp.float32, 0.5, 0.8))
    masked_scores = token_positions[None, None, :] == token_groups[:, :, None]
    steps = steps + jnp.sum(jnp.where(masked_scores, depth[:, :, None], 0.0), axis=1)
    return jnp.cumsum(steps, axis=1).astype(jnp.float32)


def draw_query_gain(key, part):
    return jax.random.uniform(jax.random.fold_in(key, 21), (HD,), jnp.float32, 0.6, 1.4)


def draw_key_gain(key, part):
    return jax.random.uniform(jax.random.fold_in(key, 31), (HD,), jnp.float32, 0.6, 1.4)


def block_scale(own_key, shape, cuts, low, largest):
    factor_of = 1.0
    for position, blocks in cuts:
        steps = jax.random.uniform(jax.random.fold_in(jax.random.fold_in(own_key, 6), position), (blocks,), jnp.float32, low / len(cuts), largest / len(cuts))
        factor_of = factor_of * jnp.repeat(jnp.exp(steps), shape[position] // blocks).reshape((-1,) + (1,) * (len(shape) - 1 - position))
    return factor_of


def routed_block(key, own, number, rows, amount, top, most, lean):
    ranking = jax.random.permutation(key, amount)
    crowded, usual = portions_of(amount, rows * top, most, lean, True), portions_of(amount, rows * top, most, lean, False)
    places = jnp.arange(amount)

    def named(tallies, rotation):
        used = int((tallies > 0).sum())
        fixed = max(1, used // 4)
        passed = fixed + (places - fixed + rotation * (used - fixed)) % max(1, amount - fixed)
        return jnp.zeros((amount,), jnp.int32).at[ranking[jnp.where(places < fixed, places, passed)]].set(jnp.asarray(tallies, jnp.int32))

    tallies = jnp.where(number % 4 == 0, named(crowded, number // 4), named(usual, number - number // 4 - 1))
    mixed = jax.random.permutation(jax.random.fold_in(own, 3), amount)
    giver, sink = mixed[0:amount // 2 * 2:2], mixed[1:amount // 2 * 2:2]
    margin = jnp.minimum(tallies[giver] - 1, most - tallies[sink]) // 2
    margin = jnp.where((giver == ranking[0]) | (sink == ranking[0]) | (tallies[sink] == 0), 0, jnp.maximum(margin, 0))
    passed = jax.random.randint(jax.random.fold_in(own, 4), (amount // 2,), 0, 1 << 20) % (margin + 1)
    tallies = tallies.at[giver].add(-passed).at[sink].add(passed)
    items = jnp.searchsorted(jnp.cumsum(tallies), jnp.arange(rows * top), side="right").astype(jnp.int32)
    grid = items.reshape(top, rows).T
    grid = grid[jax.random.permutation(jax.random.fold_in(own, 1), rows)]
    rotation = jax.random.randint(jax.random.fold_in(own, 2), (rows, 1), 0, top)
    return jnp.take_along_axis(grid, (jnp.arange(top)[None, :] + rotation) % top, axis=1)


def portions_of(number_of, total, limit, slope, full):
    loads = [(1 << 20) // math.isqrt(rank ** slope) + 1 for rank in range(1, number_of + 1)]
    largest = limit if full else min(limit, max(-(-total // number_of), total * loads[0] // sum(loads)))
    least = 1 if total - largest >= number_of - 1 else 0
    holding, spare = [largest] + [least] * (number_of - 1), total - largest - least * (number_of - 1)
    while spare > 0:
        free = [i for i in range(1, number_of) if holding[i] < largest] or [i for i in range(1, number_of) if holding[i] < limit]
        pool, left = sum([loads[i] for i in free]), spare
        for i in free:
            addition = min(limit - holding[i], max(1, left * loads[i] // pool), spare)
            holding[i] = holding[i] + addition
            spare = spare - addition
    return np.array(holding)


def scatter_about(rng, shape, deviation, limit, pieces=(), kind=jnp.bfloat16):
    drawn = deviation * jax.random.normal(rng, shape, jnp.float32)
    if pieces:
        drawn = drawn * block_scale(rng, shape, pieces, -0.22, 0.18)
    return jnp.clip(drawn, -limit, limit).astype(kind)


def setup_inputs(seed: int = 0) -> dict:
    streams_of = jax.random.split(jax.random.key(seed), 15)
    queries = scatter_about(streams_of[0], (ATTENTION_TOKENS, QUERY_HEADS * HD), 1.0, 6.0, ((0, 8), (1, 4)))
    keys = scatter_about(streams_of[1], (ATTENTION_TOKENS, KV_HEADS * HD), 1.0, 6.0, ((0, 8), (1, 4)))
    values = scatter_about(streams_of[2], (ATTENTION_TOKENS, KV_HEADS * HD), 1.0, 6.0, ((0, 8), (1, 4)))
    forget_cache = draw_forget_cache(jax.random.fold_in(streams_of[14], 71), 0)
    query_gain = draw_query_gain(jax.random.fold_in(streams_of[14], 71), 0)
    key_gain = draw_key_gain(jax.random.fold_in(streams_of[14], 71), 0)
    mixer_out = scatter_about(streams_of[6], (QUERY_HEADS * HD, D), (QUERY_HEADS * HD // 16) ** -0.5, 0.75)
    expert_input = scatter_about(streams_of[7], (TOK_B, D), 1.0, 6.0, ((0, 32),))
    norm_gain = jnp.clip(1.0 + 0.18 * jax.random.normal(streams_of[8], (D,), jnp.float32), 0.1, 1.9)
    routes_keys = jax.random.split(jax.random.fold_in(streams_of[9], 1), TOK_B // TB_DEV)
    routes_turns = jax.random.permutation(jax.random.fold_in(streams_of[9], 3), TOK_B // TB_DEV)
    routes = jax.vmap(lambda own, number: routed_block(jax.random.fold_in(streams_of[9], 2), own, number, TB_DEV, EXPERTS, TOPK, CAP, 1))(routes_keys, routes_turns).reshape((TOK_B, TOPK))
    route_weights = jnp.clip(0.1 + 0.9 * jax.random.uniform(streams_of[10], (TOK_B, TOPK), jnp.float32) ** block_scale(streams_of[10], (TOK_B, TOPK), ((0, 32),), -0.2, 0.2), 0.1, 1.0)
    w_gate = scatter_about(streams_of[11], (EXPERTS, D, FF), D ** -0.5, 0.125, ((0, 8), (2, 4)))
    w_up = scatter_about(streams_of[12], (EXPERTS, D, FF), D ** -0.5, 0.125, ((0, 8), (2, 4)))
    w_down = scatter_about(streams_of[13], (EXPERTS, D, FF), FF ** -0.5, 0.1875, ((0, 8), (2, 4)))
    return dict(queries=queries, keys=keys, values=values, forget_cache=forget_cache, query_gain=query_gain, key_gain=key_gain, mixer_out=mixer_out, expert_input=expert_input, norm_gain=norm_gain, routes=routes, route_weights=route_weights, w_gate=w_gate, w_up=w_up, w_down=w_down)


EPSILON = 1e-06
NEGATIVE = -1e+30

def rms_scale(inputs, gain):
    inputs = inputs.astype(jnp.float32)
    return inputs * lax.rsqrt(lax.optimization_barrier(jnp.mean(inputs * inputs, axis=-1, keepdims=True)) + EPSILON) * gain

def reference(queries, keys, values, forget_cache, query_gain, key_gain, mixer_out, expert_input, norm_gain, routes, route_weights, w_gate, w_up, w_down):
    total = queries.shape[0]
    group = QUERY_HEADS // KV_HEADS
    normed_q = rms_scale(queries.reshape(total, QUERY_HEADS, HD), query_gain).astype(jnp.bfloat16)
    normed_q = lax.optimization_barrier(normed_q).astype(jnp.float32)
    normed_k = rms_scale(keys.reshape(total, KV_HEADS, HD), key_gain).astype(jnp.bfloat16)
    normed_k = lax.optimization_barrier(normed_k).astype(jnp.float32)
    key_heads = jnp.repeat(normed_k, group, axis=1)
    value_heads = jnp.repeat(values.reshape(total, KV_HEADS, HD).astype(jnp.float32), group, axis=1)
    block = math.gcd(total, 512)
    token_positions = jnp.arange(total, dtype=jnp.int32)
    scale = HD ** (-0.5)

    def one_block(number):
        first = (number * block).astype(jnp.int32)
        query_block = lax.dynamic_slice_in_dim(normed_q, first, block, 0)
        scores = jnp.einsum('qhd,khd->hqk', query_block, key_heads) * scale
        gates_q = lax.dynamic_slice_in_dim(forget_cache, first, block, 1)
        scores = scores + gates_q[:, :, None] - forget_cache[:, None, :]
        allowed = token_positions[None, :] <= (first + jnp.arange(block, dtype=jnp.int32))[:, None]
        scores = jnp.where(allowed[None], scores, NEGATIVE)
        highest = lax.optimization_barrier(jnp.max(scores, axis=2, keepdims=True))
        weights = jnp.where(allowed[None], jnp.exp(scores - highest), 0.0)
        denom = lax.optimization_barrier(jnp.sum(weights, axis=2))
        rounded = lax.optimization_barrier(weights.astype(jnp.bfloat16)).astype(jnp.float32)
        numer = jnp.einsum('hqk,khd->qhd', rounded, value_heads)
        return (numer / denom.T[:, :, None]).astype(jnp.bfloat16)
    attended = lax.map(one_block, jnp.arange(total // block, dtype=jnp.int32)).reshape(total, QUERY_HEADS * HD)
    mixed = jnp.dot(attended, mixer_out, preferred_element_type=jnp.float32).astype(jnp.bfloat16)
    normed_b = rms_scale(expert_input, norm_gain).astype(jnp.bfloat16)
    count = expert_input.shape[0]
    flat = routes.reshape(-1)
    most = N_EP * N_TP * CAP
    padded = jnp.concatenate([normed_b, jnp.zeros((1, D), jnp.bfloat16)], axis=0)
    flat_weights = jnp.concatenate([route_weights.reshape(-1), jnp.zeros((1,), jnp.float32)])

    def per_expert(totals, expert):
        chosen = jnp.nonzero(flat == expert, size=most, fill_value=flat.shape[0])[0].astype(jnp.int32)
        owner = (chosen // TOPK).astype(jnp.int32)
        rows = padded[owner]
        gate = jnp.dot(rows, w_gate[expert], preferred_element_type=jnp.float32)
        upward = jnp.dot(rows, w_up[expert], preferred_element_type=jnp.float32)
        hidden = (jax.nn.silu(gate) * upward).astype(jnp.bfloat16)
        output = jnp.dot(hidden, w_down[expert].T, preferred_element_type=jnp.float32).astype(jnp.bfloat16)
        return (totals.at[owner].add(output.astype(jnp.float32) * flat_weights[chosen][:, None]), None)
    totals = lax.scan(per_expert, jnp.zeros((count + 1, D), jnp.float32), jnp.arange(EXPERTS, dtype=jnp.int32))[0]
    routed = totals[:count].astype(jnp.bfloat16)
    return (mixed, routed)
```

```python
import functools

import jax
import jax.numpy as jnp
from jax import lax
from jax.experimental import pallas as pl
from jax.experimental.pallas import tpu as pltpu
from jax.sharding import PartitionSpec as P

EXPERTS = 32
CAP = 16
CHUNKS = 2

EPSILON = 1e-06
FAR = 1e30


def rms_scale(inputs, gain):
    inputs = inputs.astype(jnp.float32)
    return inputs * lax.rsqrt(jnp.mean(inputs * inputs, axis=-1, keepdims=True) + EPSILON) * gain


def flip(value, axis, size, bit):
    return lax.ppermute(value, axis, [(i, i ^ bit) for i in range(size)])


def ffn_body(*refs, pieces):
    rows = refs[:pieces]
    gate_ref, up_ref, down_ref = refs[pieces : pieces + 3]
    outs = refs[pieces + 3 :]
    w_gate, w_up, w_down = gate_ref[0], up_ref[0], down_ref[0]
    for source, out in zip(rows, outs):
        groups, _, cap, width = source.shape
        x = source[...].reshape(groups * cap, width)
        gate = jnp.dot(x, w_gate, preferred_element_type=jnp.float32)
        upward = jnp.dot(x, w_up, preferred_element_type=jnp.float32)
        hidden = (gate / (1.0 + jnp.exp(-gate)) * upward).astype(jnp.bfloat16)
        result = lax.dot_general(
            hidden, w_down, (((1,), (1,)), ((), ())), preferred_element_type=jnp.float32
        )
        out[...] = result.astype(jnp.bfloat16).reshape(groups, 1, cap, width)


def ffn(pieces, w_gate, w_up, w_down, first):
    groups, experts, cap, width = pieces[0].shape
    hidden = w_gate.shape[2]
    row_spec = pl.BlockSpec((groups, 1, cap, width), lambda e: (0, e, 0, 0))
    in_spec = pl.BlockSpec((1, width, hidden), lambda e: (first + e, 0, 0))
    down_spec = pl.BlockSpec((1, w_down.shape[1], hidden), lambda e: (first + e, 0, 0))
    count = len(pieces)
    total = count * groups * cap * experts
    return pl.pallas_call(
        functools.partial(ffn_body, pieces=count),
        grid=(experts,),
        in_specs=[row_spec] * count + [in_spec, in_spec, down_spec],
        out_specs=[row_spec] * count,
        out_shape=[jax.ShapeDtypeStruct(pieces[0].shape, jnp.bfloat16)] * count,
        cost_estimate=pl.CostEstimate(
            flops=total * width * hidden * 6,
            bytes_accessed=experts * width * hidden * 6 + total * width * 4,
            transcendentals=total * hidden,
        ),
    )(*pieces, w_gate, w_up, w_down)


def share_keys(packed, n_ep):
    blocks = [(0, False, packed)]
    even = [(i, i + 1) for i in range(0, n_ep, 2)]
    blocks.append((0, True, lax.ppermute(packed, "ep", even)))
    for step in range(1, n_ep // 2):
        moved = lax.ppermute(
            packed, "ep", [(i, i + 2 * step) for i in range(n_ep) if i + 2 * step < n_ep]
        )
        blocks.append((step, False, moved))
        blocks.append((step, True, flip(moved, "ep", n_ep, 1)))
    return blocks


def attend(queries, keys, values, forget_cache, query_gain, key_gain, n_ep):
    rows = queries.shape[0]
    head_dim = keys.shape[1]
    heads = forget_cache.shape[0]
    place = lax.axis_index("ep")
    normed_k = rms_scale(keys, key_gain).astype(jnp.bfloat16)
    blocks = share_keys(jnp.concatenate([normed_k, values], axis=1), n_ep)
    normed_q = rms_scale(queries.reshape(rows, heads, head_dim), query_gain).astype(jnp.bfloat16)
    stacked = jnp.swapaxes(normed_q, 0, 1).reshape(heads * rows, head_dim)
    query_gates = lax.dynamic_slice_in_dim(forget_cache, place * rows, rows, 1)
    scale = head_dim ** (-0.5)
    state = None
    for step, other, block in blocks:
        number = (place - 2 * step) ^ 1 if other else place - 2 * step
        usable = (number >= 0) & (number <= place)
        begin = jnp.maximum(number, 0) * rows
        gates = lax.dynamic_slice_in_dim(forget_cache, begin, rows, 1)
        gates = jnp.where(usable, gates, FAR)
        scores = lax.dot_general(
            stacked,
            block[:, :head_dim],
            (((1,), (1,)), ((), ())),
            preferred_element_type=jnp.float32,
        ).reshape(heads, rows, rows)
        scores = scores * scale + query_gates[:, :, None] - gates[:, None, :]
        if state is None:
            index = jnp.arange(rows, dtype=jnp.int32)
            scores = jnp.where((index[None, :] <= index[:, None])[None], scores, -FAR)
        newest = jnp.max(scores, axis=2)
        if state is not None:
            newest = jnp.maximum(newest, state[0])
        weights = jnp.exp(scores - newest[:, :, None])
        total = jnp.sum(weights, axis=2)
        product = jnp.dot(
            weights.astype(jnp.bfloat16).reshape(heads * rows, rows),
            block[:, head_dim:],
            preferred_element_type=jnp.float32,
        ).reshape(heads, rows, head_dim)
        if state is not None:
            factor = jnp.exp(state[0] - newest)
            total = state[1] * factor + total
            product = state[2] * factor[:, :, None] + product
        state = (newest, total, product)
    attended = (state[2] / state[1][:, :, None]).astype(jnp.bfloat16)
    return jnp.swapaxes(attended, 0, 1).reshape(rows, heads * head_dim)


def mix(attended, mixer_out, n_tp):
    place = lax.axis_index("tp")
    rows = attended.shape[0] // n_tp
    width = attended.shape[1]
    result = 0.0
    for q in range(n_tp):
        other = place ^ q
        piece = lax.dynamic_slice_in_dim(attended, other * rows, rows, 0)
        if q:
            piece = flip(piece, "tp", n_tp, q)
        weight = lax.dynamic_slice_in_dim(mixer_out, other * width, width, 0)
        result = result + jnp.dot(piece, weight, preferred_element_type=jnp.float32)
    return result.astype(jnp.bfloat16)


def place_slots(routes, n_ep):
    flat = routes.reshape(-1)
    onehot = (flat[:, None] == jnp.arange(EXPERTS, dtype=jnp.int32)[None, :]).astype(jnp.bfloat16)
    index = jnp.arange(flat.shape[0], dtype=jnp.int32)
    earlier = (index[None, :] < index[:, None]).astype(jnp.bfloat16)
    prior = jnp.dot(earlier, onehot, preferred_element_type=jnp.float32)
    rank = jnp.sum(prior * onehot, axis=1).astype(jnp.int32)
    local = EXPERTS // n_ep
    chunks = CHUNKS if local % CHUNKS == 0 else 1
    part = local // chunks
    partner = (flat // local) ^ lax.axis_index("ep")
    inner = flat % local
    slot = ((inner // part * n_ep + partner) * part + inner % part) * CAP + rank
    return slot.reshape(routes.shape), chunks, part


def on_device(
    queries,
    keys,
    values,
    forget_cache,
    query_gain,
    key_gain,
    mixer_out,
    expert_input,
    norm_gain,
    routes,
    route_weights,
    w_gate,
    w_up,
    w_down,
    n_ep,
    n_tp,
):
    tokens, width = expert_input.shape
    top = routes.shape[1]
    normed = rms_scale(expert_input, norm_gain).astype(jnp.bfloat16)
    slot, chunks, part = place_slots(routes, n_ep)
    size = n_ep * part * CAP
    bits = [1 << b for b in range(n_tp.bit_length() - 1)]

    received = []
    for c in range(chunks):
        ids = c * size + jnp.arange(size, dtype=jnp.int32)
        chosen = sum((slot[:, k][None, :] == ids[:, None]).astype(jnp.bfloat16) for k in range(top))
        outgoing = jnp.dot(chosen, normed, preferred_element_type=jnp.float32).astype(jnp.bfloat16)
        outgoing = outgoing.reshape(n_ep, part, CAP, width)
        received.append(
            jnp.concatenate(
                [outgoing[:1]]
                + [flip(outgoing[s : s + 1], "ep", n_ep, s) for s in range(1, n_ep)],
                axis=0,
            )
        )

    attended = attend(queries, keys, values, forget_cache, query_gain, key_gain, n_ep)

    finals = []
    for c in range(chunks):
        pieces = {0: received[c]}
        for bit in reversed(bits):
            for q in list(pieces):
                pieces[q | bit] = flip(pieces[q], "tp", n_tp, bit)
        partial = {}
        half = max(1, n_tp // 2)
        for begin in range(0, n_tp, half):
            names = list(range(begin, begin + half))
            outs = ffn([pieces[q] for q in names], w_gate, w_up, w_down, c * part)
            partial.update(zip(names, outs))
        for number, bit in enumerate(bits):
            for q in sorted(partial, reverse=True):
                if q & bit:
                    continue
                came = flip(partial[q | bit], "tp", n_tp, bit)
                partial[q] = (
                    partial[q].astype(jnp.float32) + came.astype(jnp.float32)
                ).astype(jnp.bfloat16)
            partial = {q: v for q, v in partial.items() if not q & bit}
        finals.append(partial[0])

    mixed = mix(attended, mixer_out, n_tp)

    picked = [0.0] * top
    for c in range(chunks):
        final = finals[c]
        back = jnp.concatenate(
            [final[:1]] + [flip(final[s : s + 1], "ep", n_ep, s) for s in range(1, n_ep)], axis=0
        ).reshape(size, width)
        ids = c * size + jnp.arange(size, dtype=jnp.int32)
        for k in range(top):
            chosen = (slot[:, k][:, None] == ids[None, :]).astype(jnp.bfloat16)
            picked[k] = picked[k] + jnp.dot(chosen, back, preferred_element_type=jnp.float32)
    routed = sum(picked[k] * route_weights[:, k][:, None] for k in range(top))
    return (mixed, routed.astype(jnp.bfloat16))


def solution(mesh):
    in_specs = (
        P("ep", "tp"),
        P("ep", "tp"),
        P("ep", "tp"),
        P("tp", None),
        P(),
        P(),
        P(),
        P(("ep", "tp"), None),
        P(),
        P(("ep", "tp"), None),
        P(("ep", "tp"), None),
        P("ep", None, "tp"),
        P("ep", None, "tp"),
        P("ep", None, "tp"),
    )
    out_specs = (P(("ep", "tp"), None), P(("ep", "tp"), None))
    step = functools.partial(on_device, n_ep=mesh.shape["ep"], n_tp=mesh.shape["tp"])
    return jax.shard_map(
        step, mesh=mesh, in_specs=in_specs, out_specs=out_specs, check_vma=False
    )
```

```python
import functools

import jax
import jax.numpy as jnp
from jax import lax
from jax.experimental import pallas as pl
from jax.experimental.pallas import tpu as pltpu
from jax.sharding import PartitionSpec as P

EXPERTS = 32
CAP = 16
CHUNKS = 2

EPSILON = 1e-06
FAR = 1e30


def rms_scale(inputs, gain):
    inputs = inputs.astype(jnp.float32)
    return inputs * lax.rsqrt(jnp.mean(inputs * inputs, axis=-1, keepdims=True) + EPSILON) * gain


def flip(value, axis, size, bit):
    return lax.ppermute(value, axis, [(i, i ^ bit) for i in range(size)])


def ffn_body(*refs, pieces):
    rows = refs[:pieces]
    gate_ref, up_ref, down_ref = refs[pieces : pieces + 3]
    outs = refs[pieces + 3 :]
    w_gate, w_up, w_down = gate_ref[0], up_ref[0], down_ref[0]
    groups, _, cap, width = rows[0].shape
    size = groups * cap
    x = jnp.concatenate([source[...].reshape(size, width) for source in rows], axis=0)
    gate = jnp.dot(x, w_gate, preferred_element_type=jnp.float32)
    upward = jnp.dot(x, w_up, preferred_element_type=jnp.float32)
    hidden = (gate / (1.0 + jnp.exp(-gate)) * upward).astype(jnp.bfloat16)
    result = lax.dot_general(
        hidden, w_down, (((1,), (1,)), ((), ())), preferred_element_type=jnp.float32
    ).astype(jnp.bfloat16)
    for number, out in enumerate(outs):
        out[...] = result[number * size : (number + 1) * size].reshape(groups, 1, cap, width)


def join_body(*refs):
    out = refs[-1]
    for number, source in enumerate(refs[:-1]):
        out[number] = source[0]


def join(pieces):
    shape = (len(pieces),) + pieces[0].shape[1:]
    return pl.pallas_call(
        join_body,
        out_shape=jax.ShapeDtypeStruct(shape, pieces[0].dtype),
        cost_estimate=pl.CostEstimate(
            flops=0, bytes_accessed=4 * shape[0] * shape[1] * shape[2] * shape[3], transcendentals=0
        ),
    )(*pieces)


def ffn(pieces, w_gate, w_up, w_down, first):
    groups, experts, cap, width = pieces[0].shape
    hidden = w_gate.shape[2]
    row_spec = pl.BlockSpec((groups, 1, cap, width), lambda e: (0, e, 0, 0))
    in_spec = pl.BlockSpec((1, width, hidden), lambda e: (first + e, 0, 0))
    down_spec = pl.BlockSpec((1, w_down.shape[1], hidden), lambda e: (first + e, 0, 0))
    count = len(pieces)
    total = count * groups * cap * experts
    return pl.pallas_call(
        functools.partial(ffn_body, pieces=count),
        grid=(experts,),
        in_specs=[row_spec] * count + [in_spec, in_spec, down_spec],
        out_specs=[row_spec] * count,
        out_shape=[jax.ShapeDtypeStruct(pieces[0].shape, jnp.bfloat16)] * count,
        cost_estimate=pl.CostEstimate(
            flops=total * width * hidden * 6,
            bytes_accessed=experts * width * hidden * 6 + total * width * 4,
            transcendentals=total * hidden,
        ),
    )(*pieces, w_gate, w_up, w_down)


def combine_body(slot_ref, weight_ref, *refs):
    out = refs[-1]
    width = out.shape[1]
    back = jnp.concatenate([ref[...].reshape(-1, width) for ref in refs[:-1]], axis=0)
    top, tokens = slot_ref.shape[0], slot_ref.shape[1]
    ids = lax.broadcasted_iota(jnp.int32, (tokens, back.shape[0]), 1)
    total = jnp.zeros((tokens, width), jnp.float32)
    for k in range(top):
        chosen = (slot_ref[k] == ids).astype(jnp.float32).astype(jnp.bfloat16)
        total += jnp.dot(chosen, back, preferred_element_type=jnp.float32) * weight_ref[k]
    out[...] = total.astype(jnp.bfloat16)


def combine(pieces, slot, route_weights):
    tokens = slot.shape[0]
    width = pieces[0].shape[-1]
    return pl.pallas_call(
        combine_body,
        out_shape=jax.ShapeDtypeStruct((tokens, width), jnp.bfloat16),
        compiler_params=pltpu.CompilerParams(vmem_limit_bytes=40 << 20),
    )(slot.T[:, :, None], route_weights.T[:, :, None], *pieces)


def shift_keys(packed, n_ep):
    shifted = [packed]
    for step in range(1, n_ep // 2):
        pairs = [(i, i + 2 * step) for i in range(n_ep) if i + 2 * step < n_ep]
        shifted.append(lax.ppermute(packed, "ep", pairs))
    return shifted


def cross_keys(shifted, n_ep):
    even = [(i, i + 1) for i in range(0, n_ep, 2)]
    return [lax.ppermute(shifted[0], "ep", even)] + [flip(b, "ep", n_ep, 1) for b in shifted[1:]]


def attend(queries, shifted, crossed, forget_cache, query_gain):
    rows = queries.shape[0]
    heads = forget_cache.shape[0]
    head_dim = queries.shape[1] // heads
    place = lax.axis_index("ep")
    blocks = [(step, False, block) for step, block in enumerate(shifted)]
    blocks += [(step, True, block) for step, block in enumerate(crossed)]
    normed_q = rms_scale(queries.reshape(rows, heads, head_dim), query_gain).astype(jnp.bfloat16)
    stacked = jnp.swapaxes(normed_q, 0, 1).reshape(heads * rows, head_dim)
    query_gates = lax.dynamic_slice_in_dim(forget_cache, place * rows, rows, 1)
    scale = head_dim ** (-0.5)
    state = None
    for step, other, block in blocks:
        number = (place - 2 * step) ^ 1 if other else place - 2 * step
        usable = (number >= 0) & (number <= place)
        begin = jnp.maximum(number, 0) * rows
        gates = lax.dynamic_slice_in_dim(forget_cache, begin, rows, 1)
        gates = jnp.where(usable, gates, FAR)
        scores = lax.dot_general(
            stacked,
            block[:, :head_dim],
            (((1,), (1,)), ((), ())),
            preferred_element_type=jnp.float32,
        ).reshape(heads, rows, rows)
        scores = scores * scale + query_gates[:, :, None] - gates[:, None, :]
        if state is None:
            index = jnp.arange(rows, dtype=jnp.int32)
            scores = jnp.where((index[None, :] <= index[:, None])[None], scores, -FAR)
        newest = jnp.max(scores, axis=2)
        if state is not None:
            newest = jnp.maximum(newest, state[0])
        weights = jnp.exp(scores - newest[:, :, None])
        total = jnp.sum(weights, axis=2)
        product = jnp.dot(
            weights.astype(jnp.bfloat16).reshape(heads * rows, rows),
            block[:, head_dim:],
            preferred_element_type=jnp.float32,
        ).reshape(heads, rows, head_dim)
        if state is not None:
            factor = jnp.exp(state[0] - newest)
            total = state[1] * factor + total
            product = state[2] * factor[:, :, None] + product
        state = (newest, total, product)
    attended = (state[2] / state[1][:, :, None]).astype(jnp.bfloat16)
    return jnp.swapaxes(attended, 0, 1).reshape(rows, heads * head_dim)


def mix(attended, mixer_out, n_tp):
    place = lax.axis_index("tp")
    rows = attended.shape[0] // n_tp
    width = attended.shape[1]
    result = 0.0
    for q in range(n_tp):
        other = place ^ q
        piece = lax.dynamic_slice_in_dim(attended, other * rows, rows, 0)
        if q:
            piece = flip(piece, "tp", n_tp, q)
        weight = lax.dynamic_slice_in_dim(mixer_out, other * width, width, 0)
        result = result + jnp.dot(piece, weight, preferred_element_type=jnp.float32)
    return result.astype(jnp.bfloat16)


def place_slots(routes, n_ep):
    flat = routes.reshape(-1)
    onehot = (flat[:, None] == jnp.arange(EXPERTS, dtype=jnp.int32)[None, :]).astype(jnp.bfloat16)
    index = jnp.arange(flat.shape[0], dtype=jnp.int32)
    earlier = (index[None, :] < index[:, None]).astype(jnp.bfloat16)
    prior = jnp.dot(earlier, onehot, preferred_element_type=jnp.float32)
    rank = jnp.sum(prior * onehot, axis=1).astype(jnp.int32)
    local = EXPERTS // n_ep
    chunks = CHUNKS if local % CHUNKS == 0 else 1
    part = local // chunks
    partner = (flat // local) ^ lax.axis_index("ep")
    inner = flat % local
    slot = ((inner // part * n_ep + partner) * part + inner % part) * CAP + rank
    return slot.reshape(routes.shape), chunks, part


def on_device(
    queries,
    keys,
    values,
    forget_cache,
    query_gain,
    key_gain,
    mixer_out,
    expert_input,
    norm_gain,
    routes,
    route_weights,
    w_gate,
    w_up,
    w_down,
    n_ep,
    n_tp,
):
    _, width = expert_input.shape
    top = routes.shape[1]
    normed = rms_scale(expert_input, norm_gain).astype(jnp.bfloat16)
    slot, chunks, part = place_slots(routes, n_ep)
    size = n_ep * part * CAP
    bits = [1 << b for b in range(n_tp.bit_length() - 1)]

    received = []
    for c in range(chunks):
        ids = c * size + jnp.arange(size, dtype=jnp.int32)
        chosen = sum((slot[:, k][None, :] == ids[:, None]).astype(jnp.bfloat16) for k in range(top))
        outgoing = jnp.dot(chosen, normed, preferred_element_type=jnp.float32).astype(jnp.bfloat16)
        outgoing = outgoing.reshape(n_ep, part, CAP, width)
        came = [flip(outgoing[s : s + 1], "ep", n_ep, s) for s in range(1, n_ep)]
        received.append(join([outgoing[:1]] + came))

    keys, received[-1] = lax.optimization_barrier((keys, received[-1]))
    normed_k = rms_scale(keys, key_gain).astype(jnp.bfloat16)
    packed = jnp.concatenate([normed_k, values], axis=1)
    shifted = shift_keys(packed, n_ep)
    crossed = cross_keys(shifted, n_ep)

    finals = []
    for c in range(chunks):
        pieces = {0: received[c]}
        for bit in reversed(bits):
            for q in list(pieces):
                pieces[q | bit] = flip(pieces[q], "tp", n_tp, bit)
        partial = {}
        half = max(1, n_tp // 2)
        for begin in range(0, n_tp, half):
            names = list(range(begin, begin + half))
            outs = ffn([pieces[q] for q in names], w_gate, w_up, w_down, c * part)
            partial.update(zip(names, outs))
        for bit in bits:
            for q in sorted(partial, reverse=True):
                if q & bit:
                    continue
                came = flip(partial[q | bit], "tp", n_tp, bit)
                partial[q] = (
                    partial[q].astype(jnp.float32) + came.astype(jnp.float32)
                ).astype(jnp.bfloat16)
            partial = {q: v for q, v in partial.items() if not q & bit}
        finals.append(partial[0])

    queries, finals[0] = lax.optimization_barrier((queries, finals[0]))
    attended = attend(queries, shifted, crossed, forget_cache, query_gain)
    mixed = mix(attended, mixer_out, n_tp)

    pieces = []
    for c in range(chunks):
        final = finals[c]
        pieces.append(final[:1])
        pieces += [flip(final[s : s + 1], "ep", n_ep, s) for s in range(1, n_ep)]
    return (mixed, combine(pieces, slot, route_weights))


def solution(mesh):
    in_specs = (
        P("ep", "tp"),
        P("ep", "tp"),
        P("ep", "tp"),
        P("tp", None),
        P(),
        P(),
        P(),
        P(("ep", "tp"), None),
        P(),
        P(("ep", "tp"), None),
        P(("ep", "tp"), None),
        P("ep", None, "tp"),
        P("ep", None, "tp"),
        P("ep", None, "tp"),
    )
    out_specs = (P(("ep", "tp"), None), P(("ep", "tp"), None))
    n_tp = mesh.shape["tp"]
    device = functools.partial(on_device, n_ep=mesh.shape["ep"], n_tp=n_tp)

    return jax.shard_map(device, mesh=mesh, in_specs=in_specs, out_specs=out_specs, check_vma=False)
```
